256 devices in a mesh: ep: 64 (over z, y, core), tp: 4 (over x).
Axes of the slice: x: 4, y: 4, z: 8, core: 2. Of those that a mesh axis runs over, the one named last changes fastest.
Arguments:
- tokens_a: bfloat16 [8192, 2048], P('ep'), may hold values from -30 to 30
- attn_gain: float32 [2048], replicated, may hold values from 0.1 to 1.9
- w_query: bfloat16 [2048, 2048], P(None, 'tp'), may hold values from -2 to 2
- w_query_rot: bfloat16 [2048, 1024], P(None, 'tp'), may hold values from -0.125 to 0.125
- w_latent: bfloat16 [2048, 512], replicated, may hold values from -2 to 2
- w_key_rot: bfloat16 [2048, 32], replicated, may hold values from -0.125 to 0.125
- latent_gain: float32 [512], replicated, may hold values from 0.1 to 1.9
- w_key_up: bfloat16 [512, 2048], P(None, 'tp'), may hold values from -2 to 2
- w_value_up: bfloat16 [512, 2048], P(None, 'tp'), may hold values from -0.25 to 0.25
- w_output: bfloat16 [2048, 2048], P('tp'), may hold values from -0.125 to 0.125
- tokens_b: bfloat16 [16384, 2048], P('ep'), may hold values from -6 to 6
- ffn_gain: float32 [2048], replicated, may hold values from 0.1 to 1.9
- expert_ids: int32 [16384, 2], P('ep'), may hold values from 0 to 63, all different within a row; in each aligned block of 256 rows (0 to 255, 256 to 511, ...) at most 16 rows name the same one
- expert_weights: float32 [16384, 2], P('ep'), may hold values from 0.1 to 1
- w_gate: bfloat16 [64, 2048, 1024], P('ep', None, 'tp'), may hold values from -0.125 to 0.125
- w_up: bfloat16 [64, 2048, 1024], P('ep', None, 'tp'), may hold values from -0.125 to 0.125
- w_down: bfloat16 [64, 1024, 2048], P('ep', 'tp'), may hold values from -0.1875 to 0.1875
Outputs:
- mixed_a: bfloat16 [8192, 2048], P(('ep', 'tp'))
- mixed_b: bfloat16 [16384, 2048], P('ep', 'tp')
The draws below stay inside these ranges and needn't reach their ends.
Inputs may be any that keep to these rules, and one draw needn't show every extreme that they name: `expert_ids`: each row names 2 different experts. In the 256 rows of one index of ep no expert is named more than 16 times, and in some such block one expert is named exactly 16 times.
All inputs are finite; a program needn't handle non-finite values.
Results may differ from the reference program's by a relative error of at most 0.012.
Values may be sent and summed in bfloat16 or wider, within the bound.
No kernel may reach another device: no remote copies, remote signals or barrier semaphores. Data moves between devices by JAX's collectives and lax.ppermute only.
A program may use at most 192 MiB of HBM per device.

```python
import math
import jax
import jax.numpy as jnp
import numpy as np
from jax import lax

D = 2048
HEADS = 32
NOPE = 64
ROPE = 32
VD = 64
KVR = 512
FFE = 1024
TOP_K = 2
ROWS_A = 128
ROWS_B = 256
EXPERTS = 64
SEQ_A = 8192
TOKENS_B = 16384
CAP = 16
N_EP = 64
N_TP = 4


def draw_tokens_a(key, part):
    entries = jnp.clip(jax.random.normal(jax.random.fold_in(key, 11), (SEQ_A, D), jnp.float32), -6.0, 6.0)
    return entries.astype(jnp.bfloat16)


def draw_w_query(key, part):
    drawn = jnp.clip(jax.random.normal(jax.random.fold_in(key, 21), (D, HEADS * NOPE), jnp.float32), -6.0, 6.0)
    drawn = drawn * D ** (-0.5)
    return jnp.clip(drawn, -2.0, 2.0).astype(jnp.bfloat16)


def draw_w_latent(key, part):
    drawn = jnp.clip(jax.random.normal(jax.random.fold_in(key, 31), (D, KVR), jnp.float32), -6.0, 6.0)
    drawn = drawn * D ** (-0.5)
    return jnp.clip(drawn, -2.0, 2.0).astype(jnp.bfloat16)


def draw_w_key_up(key, part):
    drawn = jnp.clip(jax.random.normal(jax.random.fold_in(key, 41), (KVR, HEADS * NOPE), jnp.float32), -6.0, 6.0)
    drawn = drawn * KVR ** (-0.5)
    return jnp.clip(drawn, -2.0, 2.0).astype(jnp.bfloat16)


def block_levels(own_key, extent, cuts, low, high):
    level = 1.0
    for dim, parts in cuts:
        draws = jax.random.uniform(jax.random.fold_in(jax.random.fold_in(own_key, 6), dim), (parts,), jnp.float32, low / len(cuts), high / len(cuts))
        level = level * jnp.repeat(jnp.exp(draws), extent[dim] // parts).reshape((-1,) + (1,) * (len(extent) - 1 - dim))
    return level


def deal_out(rng, own, number, rows, amount, top, limit, skew):
    sequence = jax.random.permutation(rng, amount)
    heavy_load, usual = portions_of(amount, rows * top, limit, skew, True), portions_of(amount, rows * top, limit, skew, False)
    places = jnp.arange(amount)

    def named(tallies, turn):
        used = int((tallies > 0).sum())
        fixed = max(1, used // 4)
        moved = fixed + (places - fixed + turn * (used - fixed)) % max(1, amount - fixed)
        return jnp.zeros((amount,), jnp.int32).at[sequence[jnp.where(places < fixed, places, moved)]].set(jnp.asarray(tallies, jnp.int32))

    tallies = jnp.where(number % 4 == 0, named(heavy_load, number // 4), named(usual, number - number // 4 - 1))
    mixed = jax.random.permutation(jax.random.fold_in(own, 3), amount)
    giver, taker = mixed[0:amount // 2 * 2:2], mixed[1:amount // 2 * 2:2]
    room = jnp.minimum(tallies[giver] - 1, limit - tallies[taker]) // 2
    room = jnp.where((giver == sequence[0]) | (taker == sequence[0]) | (tallies[taker] == 0), 0, jnp.maximum(room, 0))
    moved = jax.random.randint(jax.random.fold_in(own, 4), (amount // 2,), 0, 1 << 20) % (room + 1)
    tallies = tallies.at[giver].add(-moved).at[taker].add(moved)
    labels = jnp.searchsorted(jnp.cumsum(tallies), jnp.arange(rows * top), side="right").astype(jnp.int32)
    grid = labels.reshape(top, rows).T
    grid = grid[jax.random.permutation(jax.random.fold_in(own, 1), rows)]
    turn = jax.random.randint(jax.random.fold_in(own, 2), (rows, 1), 0, top)
    return jnp.take_along_axis(grid, (jnp.arange(top)[None, :] + turn) % top, axis=1)


def portions_of(amount, total, most, lean, full):
    weights = [(1 << 20) // math.isqrt(grade ** lean) + 1 for grade in range(1, amount + 1)]
    largest = most if full else min(most, max(-(-total // amount), total * weights[0] // sum(weights)))
    least = 1 if total - largest >= amount - 1 else 0
    given, surplus = [largest] + [least] * (amount - 1), total - largest - least * (amount - 1)
    while surplus > 0:
        movable = [i for i in range(1, amount) if given[i] < largest] or [i for i in range(1, amount) if given[i] < most]
        pool, left = sum([weights[i] for i in movable]), surplus
        for i in movable:
            more = min(most - given[i], max(1, left * weights[i] // pool), surplus)
            given[i] = given[i] + more
            surplus = surplus - more
    return np.array(given)


def scatter_about(key, dims, scale, reach, cuts=(), kind=jnp.bfloat16):
    level = block_levels(key, dims, cuts, -0.22, 0.18) if cuts else 1.0
    values = jax.random.normal(key, dims, jnp.float32) * scale * level
    return jnp.minimum(jnp.maximum(values, -reach), reach).astype(kind)


def setup_inputs(seed: int = 0) -> dict:
    seeds = jax.random.split(jax.random.key(seed), 18)
    tokens_a = draw_tokens_a(jax.random.fold_in(seeds[17], 71), 0)
    attn_gain = jnp.clip(1.0 + 0.18 * jax.random.normal(seeds[1], (D,), jnp.float32), 0.1, 1.9)
    w_query = draw_w_query(jax.random.fold_in(seeds[17], 71), 0)
    w_query_rot = scatter_about(seeds[3], (D, HEADS * ROPE), D ** -0.5, 0.125, ((1, 4),))
    w_latent = draw_w_latent(jax.random.fold_in(seeds[17], 71), 0)
    w_key_rot = scatter_about(seeds[5], (D, ROPE), D ** -0.5, 0.125)
    latent_gain = jnp.clip(1.0 + 0.18 * jax.random.normal(seeds[6], (KVR,), jnp.float32), 0.1, 1.9)
    w_key_up = draw_w_key_up(jax.random.fold_in(seeds[17], 71), 0)
    w_value_up = scatter_about(seeds[8], (KVR, HEADS * VD), KVR ** -0.5, 0.25, ((1, 4),))
    w_output = scatter_about(seeds[9], (HEADS * VD, D), (HEADS * VD) ** -0.5, 0.125, ((0, 4),))
    tokens_b = scatter_about(seeds[10], (TOKENS_B, D), 1.0, 6.0, ((0, 64),))
    ffn_gain = jnp.clip(1.0 + 0.18 * jax.random.normal(seeds[11], (D,), jnp.float32), 0.1, 1.9)
    expert_ids_keys = jax.random.split(jax.random.fold_in(seeds[12], 1), TOKENS_B // ROWS_B)
    expert_ids_turns = jax.random.permutation(jax.random.fold_in(seeds[12], 3), TOKENS_B // ROWS_B)
    expert_ids = jax.vmap(lambda own, number: deal_out(jax.random.fold_in(seeds[12], 2), own, number, ROWS_B, EXPERTS, TOP_K, CAP, 1))(expert_ids_keys, expert_ids_turns).reshape((TOKENS_B, TOP_K))
    expert_weights = jnp.clip(0.1 + 0.9 * jax.random.uniform(seeds[13], (TOKENS_B, TOP_K), jnp.float32) ** block_levels(seeds[13], (TOKENS_B, TOP_K), ((0, 64),), -0.2, 0.2), 0.1, 1.0)
    w_gate = scatter_about(seeds[14], (EXPERTS, D, FFE), D ** -0.5, 0.125, ((0, 64), (2, 4)))
    w_up = scatter_about(seeds[15], (EXPERTS, D, FFE), D ** -0.5, 0.125, ((0, 64), (2, 4)))
    w_down = scatter_about(seeds[16], (EXPERTS, FFE, D), FFE ** -0.5, 0.1875, ((0, 64), (1, 4)))
    return dict(tokens_a=tokens_a, attn_gain=attn_gain, w_query=w_query, w_query_rot=w_query_rot, w_latent=w_latent, w_key_rot=w_key_rot, latent_gain=latent_gain, w_key_up=w_key_up, w_value_up=w_value_up, w_output=w_output, tokens_b=tokens_b, ffn_gain=ffn_gain, expert_ids=expert_ids, expert_weights=expert_weights, w_gate=w_gate, w_up=w_up, w_down=w_down)


epsilon = 1e-06
rope_base = 10000.0

def normalize(matrix, gain):
    floats = matrix.astype(jnp.float32)
    scaled = floats * lax.rsqrt(lax.optimization_barrier(jnp.mean(floats * floats, axis=-1, keepdims=True)) + epsilon)
    return scaled * gain.astype(jnp.float32)

def rotate(vectors, positions):
    rot_width = vectors.shape[-1]
    half_width = rot_width // 2
    inverse = rope_base ** (-(jnp.arange(half_width, dtype=jnp.float32) * 2.0) / rot_width)
    angles = positions.astype(jnp.float32)[:, None] * inverse[None, :]
    cosine = jnp.cos(angles)[:, None, :]
    sine_part = jnp.sin(angles)[:, None, :]
    first_half = vectors[..., :half_width]
    second_half = vectors[..., half_width:]
    return jnp.concatenate([first_half * cosine - second_half * sine_part, first_half * sine_part + second_half * cosine], axis=-1)

def attention_half(tokens_a, attn_gain, w_query, w_query_rot, w_latent, w_key_rot, latent_gain, w_key_up, w_value_up, w_output):
    positions = jnp.arange(SEQ_A, dtype=jnp.int32)
    normed = normalize(tokens_a, attn_gain).astype(jnp.bfloat16)
    query_plain = jnp.dot(normed, w_query, preferred_element_type=jnp.float32).astype(jnp.bfloat16)
    query_plain = query_plain.reshape(N_EP, ROWS_A, HEADS, NOPE)
    turned = jnp.dot(normed, w_query_rot, preferred_element_type=jnp.float32).reshape(SEQ_A, HEADS, ROPE)
    query_rotated_rows = rotate(turned, positions).astype(jnp.bfloat16).reshape(N_EP, ROWS_A, HEADS, ROPE)
    latent = normalize(jnp.dot(normed, w_latent, preferred_element_type=jnp.float32), latent_gain).astype(jnp.bfloat16)
    key_raw = jnp.dot(normed, w_key_rot, preferred_element_type=jnp.float32)[:, None, :]
    key_turned = rotate(key_raw, positions)[:, 0, :].astype(jnp.bfloat16)
    key_plain = jnp.dot(latent, w_key_up, preferred_element_type=jnp.float32).astype(jnp.bfloat16)
    values = jnp.dot(latent, w_value_up, preferred_element_type=jnp.float32).astype(jnp.bfloat16)
    key_wide_float = key_plain.astype(jnp.float32).reshape(N_EP, ROWS_A, HEADS, NOPE)
    rotated_key_float = key_turned.astype(jnp.float32).reshape(N_EP, ROWS_A, ROPE)
    value_float = values.astype(jnp.float32).reshape(N_EP, ROWS_A, HEADS, VD)
    key_pos = positions.reshape(N_EP, ROWS_A)
    logit_scale = (NOPE + ROPE) ** (-0.5)

    def one_block(inputs):
        query_tile_block, rotated_key_block, query_pos = inputs
        score_matrix = (jnp.einsum('yvz,wrvz->yvwr', query_tile_block.astype(jnp.float32), key_wide_float) + jnp.einsum('yjx,inx->yjin', rotated_key_block.astype(jnp.float32), rotated_key_float)) * logit_scale
        allowed = key_pos[None, None, :, :] <= query_pos[:, None, None, None]
        masked = jnp.where(allowed, score_matrix, -1e+30)
        block_max = lax.optimization_barrier(jnp.max(masked, axis=-1))
        probs = jnp.where(allowed, jnp.exp(masked - block_max[..., None]), 0.0)
        block_total = lax.optimization_barrier(jnp.sum(probs, axis=-1))
        rounded = probs.astype(jnp.bfloat16).astype(jnp.float32)
        block_out = jnp.einsum('qhbk,bkhd->qhbd', rounded, value_float)
        overall = lax.optimization_barrier(jnp.max(block_max, axis=-1))
        factor = jnp.exp(block_max - overall[..., None])
        denominator = lax.optimization_barrier(jnp.sum(factor * block_total, axis=-1))
        merged = lax.optimization_barrier(jnp.sum(factor[..., None] * block_out, axis=2))
        return (merged / denominator[..., None]).astype(jnp.bfloat16).reshape(ROWS_A, HEADS * VD)
    attended = lax.map(one_block, (query_plain, query_rotated_rows, key_pos)).reshape(SEQ_A, HEADS * VD)
    group_width = HEADS // N_TP * VD
    summed = jnp.zeros((SEQ_A, D), jnp.float32)
    for lane_index in range(N_TP):
        lane_part = jnp.dot(attended[:, lane_index * group_width:(lane_index + 1) * group_width], w_output[lane_index * group_width:(lane_index + 1) * group_width], preferred_element_type=jnp.float32)
        summed = summed + lax.optimization_barrier(lane_part.astype(jnp.bfloat16)).astype(jnp.float32)
    return summed.astype(jnp.bfloat16)

def expert_half(tokens_b, ffn_gain, expert_ids, expert_weights, w_gate, w_up, w_down):
    normed = normalize(tokens_b, ffn_gain).astype(jnp.bfloat16)
    block_pairs = ROWS_B * TOP_K
    flat_ids = expert_ids.reshape(N_EP, block_pairs)
    onehot = (flat_ids[:, :, None] == jnp.arange(EXPERTS, dtype=jnp.int32)[None, None, :]).astype(jnp.int32)
    before = jnp.cumsum(onehot, axis=1) - onehot
    slot_index = lax.optimization_barrier(jnp.sum(before * onehot, axis=2))
    block_index = jnp.arange(N_EP, dtype=jnp.int32)[:, None]
    target = (flat_ids * (N_EP * CAP) + block_index * CAP + slot_index).reshape(-1).astype(jnp.int32)
    total_slots = EXPERTS * N_EP * CAP
    pair_total = TOKENS_B * TOP_K
    source_row = jnp.zeros((total_slots,), jnp.int32).at[target].set(jnp.arange(pair_total, dtype=jnp.int32) // TOP_K)
    occupied = jnp.zeros((total_slots,), jnp.int32).at[target].set(1)
    table = source_row.reshape(EXPERTS, N_EP * CAP)
    filled = occupied.reshape(EXPERTS, N_EP * CAP)
    lane_width = FFE // N_TP

    def one_expert(inputs):
        rows_of, filled_of, gate_weight, up_weight, down_weight = inputs
        taken_rows = jnp.where(filled_of[:, None] > 0, normed[rows_of], jnp.zeros((), jnp.bfloat16))
        gate_part = jnp.dot(taken_rows, gate_weight, preferred_element_type=jnp.float32)
        up_part = jnp.dot(taken_rows, up_weight, preferred_element_type=jnp.float32)
        hidden = (jax.nn.silu(gate_part) * up_part).astype(jnp.bfloat16)
        summed = jnp.zeros((taken_rows.shape[0], D), jnp.float32)
        for lane_index in range(N_TP):
            lane_part = jnp.dot(hidden[:, lane_index * lane_width:(lane_index + 1) * lane_width], down_weight[lane_index * lane_width:(lane_index + 1) * lane_width], preferred_element_type=jnp.float32)
            summed = summed + lax.optimization_barrier(lane_part.astype(jnp.bfloat16)).astype(jnp.float32)
        return summed.astype(jnp.bfloat16)
    outputs = lax.map(one_expert, (table, filled, w_gate, w_up, w_down))
    picked = outputs.reshape(total_slots, D)[target].astype(jnp.float32).reshape(TOKENS_B, TOP_K, D)
    shares = expert_weights / lax.optimization_barrier(jnp.sum(expert_weights, axis=1, keepdims=True))
    return lax.optimization_barrier(jnp.sum(picked * shares[:, :, None], axis=1)).astype(jnp.bfloat16)

def reference(tokens_a, attn_gain, w_query, w_query_rot, w_latent, w_key_rot, latent_gain, w_key_up, w_value_up, w_output, tokens_b, ffn_gain, expert_ids, expert_weights, w_gate, w_up, w_down):
    mixed_a = attention_half(tokens_a, attn_gain, w_query, w_query_rot, w_latent, w_key_rot, latent_gain, w_key_up, w_value_up, w_output)
    mixed_b = expert_half(tokens_b, ffn_gain, expert_ids, expert_weights, w_gate, w_up, w_down)
    return (mixed_a, mixed_b)
```

```python
import functools

import jax
import jax.numpy as jnp
from jax import lax
from jax.experimental import pallas as pl
from jax.experimental.pallas import tpu as pltpu
from jax.sharding import Mesh
from jax.sharding import PartitionSpec as P


NOPE = 64
ROPE = 32
VD = 64
EPS = 1e-06
ROPE_BASE = 10000.0
F32 = jnp.float32
BF16 = jnp.bfloat16
VMEM_CAP = 60 * 1024 * 1024


def iota(shape, axis):
    return lax.broadcasted_iota(jnp.int32, shape, axis)


def dot(a, b):
    return jnp.dot(a, b, preferred_element_type=F32)


def dot_nt(a, b):
    return lax.dot_general(a, b, (((1,), (1,)), ((), ())), preferred_element_type=F32)


def params(flops=0, nbytes=0, **kw):
    return dict(
        compiler_params=pltpu.CompilerParams(vmem_limit_bytes=VMEM_CAP, **kw),
        cost_estimate=pl.CostEstimate(flops=flops, bytes_accessed=nbytes, transcendentals=0),
    )


def dispatch_kernel(t_ref, tok_ref, part_ref, gain_ref, ids_ref, *refs, capacity, experts):
    outs, tgt_ref = refs[:-1], refs[-1]
    rows = tok_ref.shape[0]
    x = tok_ref[...].astype(F32)
    inv = lax.rsqrt(jnp.mean(x * x, axis=-1, keepdims=True) + EPS)
    part = (part_ref[...].astype(F32) * inv * gain_ref[...]).astype(BF16)
    id0, id1 = ids_ref[0:1, :], ids_ref[1:2, :]
    expert = iota((experts, rows), 0)
    is0, is1 = expert == id0, expert == id1
    both = jnp.where(is0 | is1, 1.0, 0.0).astype(BF16)
    earlier = jnp.where(iota((rows, rows), 0) < iota((rows, rows), 1), 1.0, 0.0).astype(BF16)
    before = dot(both, earlier)
    slot0 = jnp.sum(jnp.where(is0, before, 0.0), axis=0, keepdims=True).astype(jnp.int32)
    slot1 = jnp.sum(jnp.where(is1, before, 0.0), axis=0, keepdims=True).astype(jnp.int32)
    chunk = capacity // len(outs)
    size = experts * chunk
    tgt0 = (slot0 // chunk) * size + id0 * chunk + slot0 % chunk
    tgt1 = (slot1 // chunk) * size + id1 * chunk + slot1 % chunk
    for c, out_ref in enumerate(outs):
        place = iota((size, rows), 0) + c * size
        sel = jnp.where((place == tgt0) | (place == tgt1), 1.0, 0.0).astype(BF16)
        out_ref[...] = dot(sel, part).astype(BF16)
    tgt_ref[...] = jnp.concatenate([tgt0, tgt1], axis=0)


def dispatch(t, tokens, gain, ids, experts, capacity, chunks, n_tp):
    rows, width = tokens.shape
    part = width // n_tp
    size = experts * capacity // chunks
    return pl.pallas_call(
        functools.partial(dispatch_kernel, capacity=capacity, experts=experts),
        grid_spec=pltpu.PrefetchScalarGridSpec(
            num_scalar_prefetch=1,
            grid=(1,),
            in_specs=[
                pl.BlockSpec((rows, width), lambda i, t: (0, 0)),
                pl.BlockSpec((rows, part), lambda i, t: (0, t[2])),
                pl.BlockSpec((1, part), lambda i, t: (0, t[2])),
                pl.BlockSpec((2, rows), lambda i, t: (0, 0)),
            ],
            out_specs=[pl.BlockSpec((size, part), lambda i, t: (0, 0))] * chunks
            + [pl.BlockSpec((2, rows), lambda i, t: (0, 0))],
        ),
        out_shape=[jax.ShapeDtypeStruct((size, part), BF16)] * chunks
        + [jax.ShapeDtypeStruct((2, rows), jnp.int32)],
        name="dispatch",
        **params(2 * rows * size * chunks * part, rows * width * 2 + size * chunks * part * 2),
    )(t, tokens, tokens, gain.reshape(1, width), ids.T)


def hidden_kernel(t_ref, x0, *refs):
    others, ws, out_ref = refs[:6], refs[6:14], refs[14]
    early = pl.program_id(0) < pl.num_programs(0) // 2
    xs = [x0[...]]
    for k in range(3):
        xs.append(jnp.where(early, others[2 * k][...], others[2 * k + 1][...]))
    gate = functools.reduce(jnp.add, [dot(x, w[...]) for x, w in zip(xs, ws[:4])])
    upp = functools.reduce(jnp.add, [dot(x, w[...]) for x, w in zip(xs, ws[4:])])
    out_ref[...] = (gate / (1.0 + jnp.exp(-gate)) * upp).astype(BF16)


def hidden_of(t, n_tp, x0, chunks, w_gate, w_up):
    rows, part = x0.shape
    width = w_gate.shape[1]
    tile = 256
    half = rows // tile // 2

    def wspec(off):
        return pl.BlockSpec((part, width), lambda i, t: (lax.rem(t[2] + off, n_tp), 0))

    row = pl.BlockSpec((tile, part), lambda i, t: (i, 0))
    first = pl.BlockSpec((tile, part), lambda i, t: (jnp.minimum(i, half - 1), 0))
    second = pl.BlockSpec((tile, part), lambda i, t: (jnp.maximum(i - half, 0), 0))
    ws = [wspec(0), wspec(n_tp - 1), wspec(1), wspec(2)]
    others = [x for pair in zip(*chunks) for x in pair]
    return pl.pallas_call(
        hidden_kernel,
        grid_spec=pltpu.PrefetchScalarGridSpec(
            num_scalar_prefetch=1,
            grid=(rows // tile,),
            in_specs=[row] + [first, second] * 3 + ws + ws,
            out_specs=pl.BlockSpec((tile, width), lambda i, t: (i, 0)),
        ),
        out_shape=jax.ShapeDtypeStruct((rows, width), BF16),
        name="hidden",
        **params(4 * rows * part * n_tp * width, rows * part * n_tp * 2),
    )(t, x0, *others, *([w_gate] * 4), *([w_up] * 4))


def columns_kernel(t_ref, w_ref, *outs):
    part = outs[0].shape[1]
    for j, out_ref in enumerate(outs):
        at = lax.rem(t_ref[2] + j, len(outs)) * part
        out_ref[...] = w_ref[:, pl.ds(pl.multiple_of(at, part), part)]


def columns_of(t, w, n_tp):
    rows, width = w.shape
    vmem = pl.BlockSpec(memory_space=pltpu.VMEM)
    return pl.pallas_call(
        columns_kernel,
        in_specs=[pl.BlockSpec(memory_space=pltpu.SMEM), vmem],
        out_specs=[vmem] * n_tp,
        out_shape=[jax.ShapeDtypeStruct((rows, width // n_tp), BF16)] * n_tp,
        name="columns",
        **params(rows * width, rows * width * 4),
    )(t, w)


def down_kernel(h0, hb, ha, fa, fb, w0, wb, wa, wf, out_ref):
    out = dot(h0[...], w0[...]) + dot(hb[...], wb[...]) + dot(ha[...], wa[...])
    half = fa.shape[0]
    out_ref[:half, :] = (out[:half] + dot(fa[...], wf[...])).astype(BF16)
    out_ref[half:, :] = (out[half:] + dot(fb[...], wf[...])).astype(BF16)


def down_of(h0, hb, ha, fa, fb, wd):
    rows, width = h0.shape
    part = wd[0].shape[1]
    return pl.pallas_call(
        down_kernel,
        out_shape=jax.ShapeDtypeStruct((rows, part), BF16),
        name="down",
        **params(2 * rows * part * len(wd) * width, rows * part * len(wd) * 2),
    )(h0, hb, ha, fa, fb, wd[0], wd[1], wd[3], wd[2])


def shares_kernel(tgt_ref, w_ref, high_ref, low_ref):
    w = w_ref[...]
    w0, w1 = w[:, 0:1], w[:, 1:2]
    total = w0 + w1
    tgt = tgt_ref[...]
    place = iota(high_ref.shape, 1)
    share = jnp.where(place == tgt[:, 0:1], w0 / total, 0.0)
    share = share + jnp.where(place == tgt[:, 1:2], w1 / total, 0.0)
    high = share.astype(BF16)
    high_ref[...] = high
    low_ref[...] = (share - high.astype(F32)).astype(BF16)


def shares_of(tgt, weights, slots):
    rows = tgt.shape[0]
    return pl.pallas_call(
        shares_kernel,
        out_shape=[jax.ShapeDtypeStruct((rows, slots), BF16)] * 2,
        name="shares",
        **params(8 * rows * slots, rows * slots * 4),
    )(tgt, weights)


def combine_kernel(ret_ref, high_ref, low_ref, out_ref):
    ret = ret_ref[...]
    out_ref[...] = (dot(high_ref[...], ret) + dot(low_ref[...], ret)).astype(BF16)


def combine(returned, high, low):
    rows = high.shape[0]
    slots, part = returned.shape
    return pl.pallas_call(
        combine_kernel,
        out_shape=jax.ShapeDtypeStruct((rows, part), BF16),
        name="combine",
        **params(4 * rows * slots * part, slots * part * 2),
    )(returned, high, low)


def project_kernel(
    tok_ref, gain_ref, wq_ref, wqr_ref, wl_ref, wkr_ref, lgain_ref, cos_ref, sin_ref, q_ref, kv_ref
):
    x = tok_ref[...].astype(F32)
    inv = lax.rsqrt(jnp.mean(x * x, axis=-1, keepdims=True) + EPS)
    normed = (x * inv * gain_ref[...]).astype(BF16)
    plain = wq_ref.shape[1]
    ranks = wl_ref.shape[1]
    cos, sin = cos_ref[...], sin_ref[...]

    def turn(v):
        n = v.shape[1]
        first = iota(v.shape, 1) % ROPE < ROPE // 2
        other = jnp.where(
            first, pltpu.roll(v, n - ROPE // 2, axis=1), pltpu.roll(v, ROPE // 2, axis=1)
        )
        return v * cos[:, :n] + other * sin[:, :n]

    q_ref[:, :plain] = dot(normed, wq_ref[...]).astype(BF16)
    q_ref[:, plain:] = turn(dot(normed, wqr_ref[...])).astype(BF16)
    raw = dot(normed, wl_ref[...])
    linv = lax.rsqrt(jnp.mean(raw * raw, axis=-1, keepdims=True) + EPS)
    kv_ref[:, :ranks] = (raw * linv * lgain_ref[...]).astype(BF16)
    key = dot_nt(normed, wkr_ref[...])
    key = jnp.concatenate([key, jnp.zeros((key.shape[0], 128 - ROPE), F32)], axis=1)
    kv_ref[:, ranks:] = turn(key).astype(BF16)


def project(tokens, gain, wq, wqr, wl, wkr, lgain, cos, sin):
    rows, width = tokens.shape
    q_width = wq.shape[1] + wqr.shape[1]
    total = q_width + wl.shape[1] + ROPE
    return pl.pallas_call(
        project_kernel,
        out_shape=[
            jax.ShapeDtypeStruct((rows, q_width), BF16),
            jax.ShapeDtypeStruct((rows, wl.shape[1] + 128), BF16),
        ],
        name="project",
        **params(2 * rows * width * total, width * total * 2),
    )(tokens, gain.reshape(1, width), wq, wqr, wl, wkr.T, lgain.reshape(1, -1), cos, sin)


def expand_kernel(wk_ref, wv_ref, *refs, heads):
    ks, (k_out, v_out) = refs[:-2], refs[-2:]
    block = ks[0].shape[0]
    ranks = wk_ref.shape[0]
    one = jnp.ones((block, 128 - VD), BF16)
    for j, k_ref in enumerate(ks):
        rows = pl.ds(j * block, block)
        lat = k_ref[:, :ranks]
        kp = dot(lat, wk_ref[...]).astype(BF16)
        vp = dot(lat, wv_ref[...]).astype(BF16)
        tail = k_ref[:, ranks:ranks + 128 - NOPE]
        for h in range(heads):
            k_out[h, rows, :] = jnp.concatenate([kp[:, h * NOPE:(h + 1) * NOPE], tail], axis=1)
            v_out[h, rows, :] = jnp.concatenate([vp[:, h * VD:(h + 1) * VD], one], axis=1)


def expand(ks, wk, wv):
    block = ks[0].shape[0]
    heads = wk.shape[1] // NOPE
    keys = block * len(ks)
    return pl.pallas_call(
        functools.partial(expand_kernel, heads=heads),
        out_shape=[jax.ShapeDtypeStruct((heads, keys, 128), BF16)] * 2,
        name="expand",
        **params(4 * keys * wk.size, keys * heads * 512),
    )(wk, wv, *ks)


def flash_kernel(at_ref, ka_ref, kb_ref, va_ref, vb_ref, *refs, heads, n_lo, n_hi, shifts):
    qs, out_ref = refs[:n_lo // 2], refs[n_lo // 2]
    q_scr, o_scr, lse_scr, bias = refs[n_lo // 2 + 1:]
    h = pl.program_id(0)
    hi, lo = at_ref[0], at_ref[1]
    block = qs[0].shape[1]
    tile = 2 * block
    n_y = n_lo // 2
    scale = (NOPE + ROPE) ** (-0.5)

    def place(i, m):
        row = lax.rem(lo // 2 - (0, 1, n_y - 1, 2)[i] + n_y, n_y)
        side = lax.rem(lo, 2)
        return row * 2 + (1 - side if m else side)

    @pl.when(h == 0)
    def _():
        lse_scr[...] = jnp.zeros_like(lse_scr)
        zero = jnp.zeros((block, 128 - NOPE - ROPE), BF16)
        gap = iota((block, block), 0) - iota((block, block), 1)
        for i in range(n_y):
            for m in range(2):
                rows = pl.ds(i * tile + m * block, block)
                for g in range(heads):
                    base = heads * NOPE + g * ROPE
                    plain = qs[i][m, :, g * NOPE:(g + 1) * NOPE]
                    turned = qs[i][m, :, base:base + ROPE]
                    q_scr[g, rows, :] = jnp.concatenate([plain, turned, zero], axis=1)
                first = hi * n_lo + place(i, m)
                for k, j in enumerate(shifts):
                    ahead = (lax.rem(hi - j + n_hi, n_hi) * n_lo + lo - first) * block
                    bias[rows, k * block:(k + 1) * block] = jnp.where(gap >= ahead, 0.0, -1e30)

    keys = jnp.concatenate([ka_ref[0], kb_ref[0]], axis=0)
    values = jnp.concatenate([va_ref[0], vb_ref[0]], axis=0)
    lane = iota((tile, 128), 1)
    for i in range(n_y):
        rows = pl.ds(i * tile, tile)
        s = dot_nt(q_scr[h, rows, :], keys) + bias[rows, :]
        top = jnp.max(s, axis=1, keepdims=True)
        p = jnp.exp2((s - top) * (scale * 1.4426950408889634)).astype(BF16)
        o = dot(p, values)
        total = o[:, VD:VD + 1]
        o_scr[h, rows, :] = (o * (1.0 / total)).astype(BF16)
        lse_scr[rows, :] = jnp.where(lane == h, top * scale + jnp.log(total), lse_scr[rows, :])

    @pl.when(h == heads - 1)
    def _():
        for i in range(n_y):
            for m in range(2):
                rows = pl.ds(i * tile + m * block, block)
                to = place(i, m)
                for g in range(heads):
                    out_ref[to, :, g * VD:(g + 1) * VD] = o_scr[g, rows, :VD]
                lse = lse_scr[rows, :]
                a = lse.astype(BF16).astype(F32)
                b = (lse - a).astype(BF16).astype(F32)
                c = lse - a - b
                packed = a + pltpu.roll(b, heads, axis=1) + pltpu.roll(c, 2 * heads, axis=1)
                out_ref[to, :, heads * VD:] = packed.astype(BF16)


def flash(at, qs, kx, vx, shifts):
    heads, keys, _ = kx[0].shape
    block = qs[0].shape[1]
    n_lo, n_hi = 2 * len(qs), len(shifts)
    rows = block * n_lo
    pair = pl.BlockSpec(qs[0].shape, lambda h, p: (0, 0, 0))
    shape = (n_lo, block, heads * VD + 128)
    return pl.pallas_call(
        functools.partial(flash_kernel, heads=heads, n_lo=n_lo, n_hi=n_hi, shifts=shifts),
        grid_spec=pltpu.PrefetchScalarGridSpec(
            num_scalar_prefetch=1,
            grid=(heads,),
            in_specs=[pl.BlockSpec((1, keys, 128), lambda h, p: (h, 0, 0))] * 4 + [pair] * len(qs),
            out_specs=pl.BlockSpec(shape, lambda h, p: (0, 0, 0)),
            scratch_shapes=[
                pltpu.VMEM((heads, rows, 128), BF16),
                pltpu.VMEM((heads, rows, 128), BF16),
                pltpu.VMEM((rows, 128), F32),
                pltpu.VMEM((rows, 2 * keys), F32),
            ],
        ),
        out_shape=jax.ShapeDtypeStruct(shape, BF16),
        name="flash",
        **params(8 * rows * keys * heads * 128, (rows * 2 + keys) * 640 * 2),
    )(at, *kx, *vx, *qs)


def merge_kernel(t_ref, parts_ref, wo_ref, *refs, heads):
    outs, scr = refs[:-1], refs[-1]
    n, rows = parts_ref.shape[:2]
    width = heads * VD
    lses = []
    for c in range(n):
        s = parts_ref[c, :, width:].astype(F32)
        lses.append(s + pltpu.roll(s, 128 - heads, axis=1) + pltpu.roll(s, 128 - 2 * heads, axis=1))
    top = functools.reduce(jnp.maximum, lses)
    factors = [jnp.exp(v - top) for v in lses]
    total = functools.reduce(jnp.add, factors)
    wide = jnp.where(iota((128, width), 1) // VD == iota((128, width), 0), 1.0, 0.0).astype(BF16)
    acc = jnp.zeros((rows, width), F32)
    for c in range(n):
        factor = factors[c] / total
        high = factor.astype(BF16)
        low = (factor - high.astype(F32)).astype(BF16)
        acc = acc + parts_ref[c, :, :width].astype(F32) * (dot(high, wide) + dot(low, wide))
    scr[...] = acc.astype(BF16)
    some = outs[0].shape[0]
    for j, out_ref in enumerate(outs):
        at = lax.rem(t_ref[2] + j, len(outs)) * some
        part = scr[pl.ds(pl.multiple_of(at, some), some), :]
        out_ref[...] = dot(part, wo_ref[...]).astype(BF16)


def merge(at, parts, wo, heads, n_tp):
    rows, width = parts.shape[1], wo.shape[1]
    vmem = pl.BlockSpec(memory_space=pltpu.VMEM)
    return pl.pallas_call(
        functools.partial(merge_kernel, heads=heads),
        in_specs=[pl.BlockSpec(memory_space=pltpu.SMEM)] + [vmem] * 2,
        out_specs=[vmem] * n_tp,
        out_shape=[jax.ShapeDtypeStruct((rows // n_tp, width), BF16)] * n_tp,
        scratch_shapes=[pltpu.VMEM((rows, heads * VD), BF16)],
        name="merge",
        **params(2 * rows * wo.shape[0] * width, wo.size * 2),
    )(at, parts, wo)


CHUNKS = 2


def round_tp(xs, n):
    up = [(i, (i + 1) % n) for i in range(n)]
    down = [(i, (i - 1) % n) for i in range(n)]
    sets = []
    for c, x in enumerate(xs):
        below = lax.ppermute(x, "tp", up)
        above = lax.ppermute(x, "tp", down)
        far = lax.ppermute(below, "tp", up) if c % 2 == 0 else lax.ppermute(above, "tp", down)
        sets.append((x, below, above, far))
    return sets


def swap_tp(xs, n):
    got = [xs[0]]
    for j in range(1, n):
        got.append(lax.ppermute(xs[j], "tp", [(i, (i + j) % n) for i in range(n)]))
    return got


def on_device(
    sizes,
    tokens_a,
    attn_gain,
    w_query,
    w_query_rot,
    w_latent,
    w_key_rot,
    latent_gain,
    w_key_up,
    w_value_up,
    w_output,
    tokens_b,
    ffn_gain,
    expert_ids,
    expert_weights,
    w_gate,
    w_up,
    w_down,
):
    n_hi, n_lo, n_tp = sizes
    n_ep = n_hi * n_lo
    hi, lo, tp = lax.axis_index("hi"), lax.axis_index("lo"), lax.axis_index("tp")
    at = jnp.stack([hi, lo, tp]).astype(jnp.int32)
    ep_axes = ("hi", "lo")

    rows_b, width = tokens_b.shape
    capacity = 2 * rows_b * expert_ids.shape[1] // n_ep
    part = width // n_tp
    outgoing, tgt = dispatch(at, tokens_b, ffn_gain, expert_ids, n_ep, capacity, 1, n_tp)
    arrived = lax.all_to_all(outgoing.reshape(n_ep, capacity, part), ep_axes, 0, 0, tiled=True)
    arrived = arrived.reshape(-1, part)

    wd = columns_of(at, w_down[0], n_tp)
    wd = swap_tp(wd, n_tp)

    rows_a = tokens_a.shape[0]
    heads = w_query.shape[1] // NOPE
    pos = ((hi * n_lo + lo) * rows_a + jnp.arange(rows_a, dtype=jnp.int32)).astype(F32)
    lane = jnp.arange(heads * ROPE, dtype=jnp.int32)
    half = ROPE // 2
    inverse = ROPE_BASE ** (-((lane % half).astype(F32) * 2.0) / ROPE)
    angles = pos[:, None] * inverse[None, :]
    cos = jnp.cos(angles)
    sin = jnp.where(lane % ROPE < half, -1.0, 1.0)[None, :] * jnp.sin(angles)
    q, kv = project(
        tokens_a, attn_gain, w_query, w_query_rot, w_latent, w_key_rot, latent_gain, cos, sin
    )

    other = [(i, i ^ 1) for i in range(n_lo)]
    up = [(i, (i + 2) % n_lo) for i in range(n_lo)]
    down = [(i, (i - 2) % n_lo) for i in range(n_lo)]
    q_other = lax.ppermute(q, "lo", other)
    pair = jnp.stack([q, q_other])
    q_below = lax.ppermute(pair, "lo", up)
    q_above = lax.ppermute(pair, "lo", down)
    q_far = lax.ppermute(q_below, "lo", up)

    def shifted(x, by):
        return lax.ppermute(x, "hi", [(i, (i + by) % n_hi) for i in range(n_hi)])

    ks = {0: kv}
    moves = ((1, 0, 1), (7, 0, -1), (2, 1, 1), (6, 7, -1), (3, 2, 1), (5, 6, -1), (4, 6, -2))
    for to, source, by in moves:
        ks[to] = shifted(ks[source], by)

    size = arrived.shape[0] // CHUNKS
    pieces = [arrived[c * size:(c + 1) * size] for c in range(CHUNKS)]
    chunks = [xs[1:] for xs in round_tp(pieces, n_tp)]
    h0 = hidden_of(at, n_tp, arrived, chunks, w_gate[0], w_up[0])
    t_up = [(i, (i + 1) % n_tp) for i in range(n_tp)]
    t_down = [(i, (i - 1) % n_tp) for i in range(n_tp)]
    hb = lax.ppermute(h0, "tp", t_up)
    ha = lax.ppermute(h0, "tp", t_down)
    fa = lax.ppermute(hb[:size], "tp", t_up)
    fb = lax.ppermute(ha[size:], "tp", t_down)
    done = down_of(h0, hb, ha, fa, fb, wd).reshape(n_ep, capacity, part)
    returned = lax.all_to_all(done, ep_axes, 0, 0, tiled=True).reshape(-1, part)
    high, low = shares_of(tgt.T, expert_weights, n_ep * capacity)
    mixed_b = combine(returned, high, low)

    near, rest = (0, 1, 7, 2), (6, 3, 5, 4)
    ka, va = expand([ks[j] for j in near], w_key_up, w_value_up)
    kb, vb = expand([ks[j] for j in rest], w_key_up, w_value_up)
    outs = flash(at, [pair, q_below, q_above, q_far], (ka, kb), (va, vb), near + rest)
    parts = lax.all_to_all(outs, "lo", 0, 0, tiled=True)
    partial = merge(at, parts, w_output, heads, n_tp)
    shared = swap_tp(partial, n_tp)
    mixed_a = functools.reduce(jnp.add, [v.astype(F32) for v in shared]).astype(BF16)
    return mixed_a, mixed_b


def solution(mesh):
    n_ep, n_tp = mesh.shape["ep"], mesh.shape["tp"]
    n_lo = 8
    n_hi = n_ep // n_lo
    grid = Mesh(mesh.devices.reshape(n_hi, n_lo, n_tp), ("hi", "lo", "tp"))
    ep = ("hi", "lo")
    placed = (
        P(ep, None),
        P(),
        P(None, "tp"),
        P(None, "tp"),
        P(),
        P(),
        P(),
        P(None, "tp"),
        P(None, "tp"),
        P("tp", None),
        P(ep, None),
        P(),
        P(ep, None),
        P(ep, None),
        P(ep, None, "tp"),
        P(ep, None, "tp"),
        P(ep, "tp", None),
    )

    def body(*args):
        return on_device((n_hi, n_lo, n_tp), *args)

    return jax.shard_map(
        body,
        mesh=grid,
        in_specs=placed,
        out_specs=(P(("hi", "lo", "tp"), None), P(ep, "tp")),
        check_vma=False,
    )
```

```python
import functools

import jax
import jax.numpy as jnp
from jax import lax
from jax.experimental import pallas as pl
from jax.experimental.pallas import tpu as pltpu
from jax.sharding import Mesh
from jax.sharding import PartitionSpec as P


NOPE = 64
ROPE = 32
VD = 64
EPS = 1e-06
ROPE_BASE = 10000.0
F32 = jnp.float32
BF16 = jnp.bfloat16
VMEM_CAP = 60 * 1024 * 1024
VMEM_ALL = 67043328


def iota(shape, axis):
    return lax.broadcasted_iota(jnp.int32, shape, axis)


def dot(a, b):
    return jnp.dot(a, b, preferred_element_type=F32)


def dot_nt(a, b):
    return lax.dot_general(a, b, (((1,), (1,)), ((), ())), preferred_element_type=F32)


def params(flops=0, nbytes=0, cap=VMEM_CAP):
    return dict(
        compiler_params=pltpu.CompilerParams(vmem_limit_bytes=cap),
        cost_estimate=pl.CostEstimate(flops=flops, bytes_accessed=nbytes, transcendentals=0),
    )


def dispatch_kernel(t_ref, tok_ref, part_ref, gain_ref, ids_ref, *refs, capacity, experts):
    outs, tgt_ref = refs[:-1], refs[-1]
    rows = tok_ref.shape[0]
    x = tok_ref[...].astype(F32)
    inv = lax.rsqrt(jnp.mean(x * x, axis=-1, keepdims=True) + EPS)
    part = (part_ref[...].astype(F32) * inv * gain_ref[...]).astype(BF16)
    id0, id1 = ids_ref[0:1, :], ids_ref[1:2, :]
    expert = iota((experts, rows), 0)
    is0, is1 = expert == id0, expert == id1
    both = jnp.where(is0 | is1, 1.0, 0.0).astype(BF16)
    earlier = jnp.where(iota((rows, rows), 0) < iota((rows, rows), 1), 1.0, 0.0).astype(BF16)
    before = dot(both, earlier)
    slot0 = jnp.sum(jnp.where(is0, before, 0.0), axis=0, keepdims=True).astype(jnp.int32)
    slot1 = jnp.sum(jnp.where(is1, before, 0.0), axis=0, keepdims=True).astype(jnp.int32)
    chunk = capacity // len(outs)
    size = experts * chunk
    tgt0 = (slot0 // chunk) * size + id0 * chunk + slot0 % chunk
    tgt1 = (slot1 // chunk) * size + id1 * chunk + slot1 % chunk
    for c, out_ref in enumerate(outs):
        place = iota((size, rows), 0) + c * size
        sel = jnp.where((place == tgt0) | (place == tgt1), 1.0, 0.0).astype(BF16)
        out_ref[...] = dot(sel, part).astype(BF16)
    tgt_ref[...] = jnp.concatenate([tgt0, tgt1], axis=0)


def dispatch(t, tokens, gain, ids, experts, capacity, chunks, n_tp):
    rows, width = tokens.shape
    part = width // n_tp
    size = experts * capacity // chunks
    return pl.pallas_call(
        functools.partial(dispatch_kernel, capacity=capacity, experts=experts),
        grid_spec=pltpu.PrefetchScalarGridSpec(
            num_scalar_prefetch=1,
            grid=(1,),
            in_specs=[
                pl.BlockSpec((rows, width), lambda i, t: (0, 0)),
                pl.BlockSpec((rows, part), lambda i, t: (0, t[2])),
                pl.BlockSpec((1, part), lambda i, t: (0, t[2])),
                pl.BlockSpec((2, rows), lambda i, t: (0, 0)),
            ],
            out_specs=[pl.BlockSpec((size, part), lambda i, t: (0, 0))] * chunks
            + [pl.BlockSpec((2, rows), lambda i, t: (0, 0))],
        ),
        out_shape=[jax.ShapeDtypeStruct((size, part), BF16)] * chunks
        + [jax.ShapeDtypeStruct((2, rows), jnp.int32)],
        name="dispatch",
        **params(2 * rows * size * chunks * part, rows * width * 2 + size * chunks * part * 2),
    )(t, tokens, tokens, gain.reshape(1, width), ids.T)


def hidden_kernel(t_ref, x0, *refs):
    others, ws, out_ref = refs[:6], refs[6:14], refs[14]
    early = pl.program_id(0) < pl.num_programs(0) // 2
    xs = [x0[...]]
    for k in range(3):
        xs.append(jnp.where(early, others[2 * k][...], others[2 * k + 1][...]))
    gate = functools.reduce(jnp.add, [dot(x, w[...]) for x, w in zip(xs, ws[:4])])
    upp = functools.reduce(jnp.add, [dot(x, w[...]) for x, w in zip(xs, ws[4:])])
    out_ref[...] = (gate / (1.0 + jnp.exp(-gate)) * upp).astype(BF16)


def hidden_of(t, n_tp, x0, chunks, w_gate, w_up):
    rows, part = x0.shape
    width = w_gate.shape[1]
    tile = 256
    half = rows // tile // 2

    def wspec(off):
        return pl.BlockSpec((part, width), lambda i, t: (lax.rem(t[2] + off, n_tp), 0))

    row = pl.BlockSpec((tile, part), lambda i, t: (i, 0))
    first = pl.BlockSpec((tile, part), lambda i, t: (jnp.minimum(i, half - 1), 0))
    second = pl.BlockSpec((tile, part), lambda i, t: (jnp.maximum(i - half, 0), 0))
    ws = [wspec(0), wspec(n_tp - 1), wspec(1), wspec(2)]
    others = [x for pair in zip(*chunks) for x in pair]
    return pl.pallas_call(
        hidden_kernel,
        grid_spec=pltpu.PrefetchScalarGridSpec(
            num_scalar_prefetch=1,
            grid=(rows // tile,),
            in_specs=[row] + [first, second] * 3 + ws + ws,
            out_specs=pl.BlockSpec((tile, width), lambda i, t: (i, 0)),
        ),
        out_shape=jax.ShapeDtypeStruct((rows, width), BF16),
        name="hidden",
        **params(4 * rows * part * n_tp * width, rows * part * n_tp * 2),
    )(t, x0, *others, *([w_gate] * 4), *([w_up] * 4))


def columns_kernel(t_ref, w_ref, *outs):
    part = outs[0].shape[1]
    for j, out_ref in enumerate(outs):
        at = lax.rem(t_ref[2] + j, len(outs)) * part
        out_ref[...] = w_ref[:, pl.ds(pl.multiple_of(at, part), part)]


def columns_of(t, w, n_tp):
    rows, width = w.shape
    vmem = pl.BlockSpec(memory_space=pltpu.VMEM)
    return pl.pallas_call(
        columns_kernel,
        in_specs=[pl.BlockSpec(memory_space=pltpu.SMEM), vmem],
        out_specs=[vmem] * n_tp,
        out_shape=[jax.ShapeDtypeStruct((rows, width // n_tp), BF16)] * n_tp,
        name="columns",
        **params(rows * width, rows * width * 4),
    )(t, w)


def down_kernel(h0, hb, ha, fa, fb, w0, wb, wa, wf, out_ref):
    out = dot(h0[...], w0[...]) + dot(hb[...], wb[...]) + dot(ha[...], wa[...])
    half = fa.shape[0]
    out_ref[:half, :] = (out[:half] + dot(fa[...], wf[...])).astype(BF16)
    out_ref[half:, :] = (out[half:] + dot(fb[...], wf[...])).astype(BF16)


def down_of(h0, hb, ha, fa, fb, wd):
    rows, width = h0.shape
    part = wd[0].shape[1]
    return pl.pallas_call(
        down_kernel,
        out_shape=jax.ShapeDtypeStruct((rows, part), BF16),
        name="down",
        **params(2 * rows * part * len(wd) * width, rows * part * len(wd) * 2),
    )(h0, hb, ha, fa, fb, wd[0], wd[1], wd[3], wd[2])


def shares_kernel(tgt_ref, w_ref, high_ref, low_ref):
    w = w_ref[...]
    w0, w1 = w[:, 0:1], w[:, 1:2]
    total = w0 + w1
    tgt = tgt_ref[...]
    place = iota(high_ref.shape, 1)
    share = jnp.where(place == tgt[:, 0:1], w0 / total, 0.0)
    share = share + jnp.where(place == tgt[:, 1:2], w1 / total, 0.0)
    high = share.astype(BF16)
    high_ref[...] = high
    low_ref[...] = (share - high.astype(F32)).astype(BF16)


def shares_of(tgt, weights, slots):
    rows = tgt.shape[0]
    return pl.pallas_call(
        shares_kernel,
        out_shape=[jax.ShapeDtypeStruct((rows, slots), BF16)] * 2,
        name="shares",
        **params(8 * rows * slots, rows * slots * 4),
    )(tgt, weights)


def combine_kernel(ret_ref, high_ref, low_ref, out_ref):
    ret = ret_ref[...]
    out_ref[...] = (dot(high_ref[...], ret) + dot(low_ref[...], ret)).astype(BF16)


def combine(returned, high, low):
    rows = high.shape[0]
    slots, part = returned.shape
    tile = 256
    share = pl.BlockSpec((rows, slots), lambda i: (0, 0))
    return pl.pallas_call(
        combine_kernel,
        grid=(part // tile,),
        in_specs=[pl.BlockSpec((slots, tile), lambda i: (0, i)), share, share],
        out_specs=pl.BlockSpec((rows, tile), lambda i: (0, i)),
        out_shape=jax.ShapeDtypeStruct((rows, part), BF16),
        name="combine",
        **params(4 * rows * slots * part, slots * part * 2, cap=VMEM_ALL),
    )(returned, high, low)


def project_kernel(
    tok_ref, gain_ref, wq_ref, wqr_ref, wl_ref, wkr_ref, lgain_ref, cos_ref, sin_ref, q_ref, kv_ref
):
    x = tok_ref[...].astype(F32)
    inv = lax.rsqrt(jnp.mean(x * x, axis=-1, keepdims=True) + EPS)
    normed = (x * inv * gain_ref[...]).astype(BF16)
    plain = wq_ref.shape[1]
    ranks = wl_ref.shape[1]
    cos, sin = cos_ref[...], sin_ref[...]

    def turn(v):
        n = v.shape[1]
        first = iota(v.shape, 1) % ROPE < ROPE // 2
        other = jnp.where(
            first, pltpu.roll(v, n - ROPE // 2, axis=1), pltpu.roll(v, ROPE // 2, axis=1)
        )
        return v * cos[:, :n] + other * sin[:, :n]

    q_ref[:, :plain] = dot(normed, wq_ref[...]).astype(BF16)
    q_ref[:, plain:] = turn(dot(normed, wqr_ref[...])).astype(BF16)
    raw = dot(normed, wl_ref[...])
    linv = lax.rsqrt(jnp.mean(raw * raw, axis=-1, keepdims=True) + EPS)
    kv_ref[:, :ranks] = (raw * linv * lgain_ref[...]).astype(BF16)
    key = dot_nt(normed, wkr_ref[...])
    key = jnp.concatenate([key, jnp.zeros((key.shape[0], 128 - ROPE), F32)], axis=1)
    kv_ref[:, ranks:] = turn(key).astype(BF16)


def project(tokens, gain, wq, wqr, wl, wkr, lgain, cos, sin):
    rows, width = tokens.shape
    q_width = wq.shape[1] + wqr.shape[1]
    total = q_width + wl.shape[1] + ROPE
    return pl.pallas_call(
        project_kernel,
        out_shape=[
            jax.ShapeDtypeStruct((rows, q_width), BF16),
            jax.ShapeDtypeStruct((rows, wl.shape[1] + 128), BF16),
        ],
        name="project",
        **params(2 * rows * width * total, width * total * 2),
    )(tokens, gain.reshape(1, width), wq, wqr, wl, wkr.T, lgain.reshape(1, -1), cos, sin)


def expand_kernel(wk_ref, wv_ref, *refs, heads):
    ks, (k_out, v_out) = refs[:-2], refs[-2:]
    block = ks[0].shape[0]
    ranks = wk_ref.shape[0]
    one = jnp.ones((block, 128 - VD), BF16)
    for j, k_ref in enumerate(ks):
        rows = pl.ds(j * block, block)
        lat = k_ref[:, :ranks]
        kp = dot(lat, wk_ref[...]).astype(BF16)
        vp = dot(lat, wv_ref[...]).astype(BF16)
        tail = k_ref[:, ranks:ranks + 128 - NOPE]
        for h in range(heads):
            k_out[h, rows, :NOPE] = kp[:, h * NOPE:(h + 1) * NOPE]
            k_out[h, rows, NOPE:] = tail
            v_out[h, rows, :VD] = vp[:, h * VD:(h + 1) * VD]
            v_out[h, rows, VD:] = one


def expand(ks, wk, wv):
    block = ks[0].shape[0]
    heads = wk.shape[1] // NOPE
    keys = block * len(ks)
    return pl.pallas_call(
        functools.partial(expand_kernel, heads=heads),
        out_shape=[jax.ShapeDtypeStruct((heads, keys, 128), BF16)] * 2,
        name="expand",
        **params(4 * keys * wk.size, keys * heads * 512),
    )(wk, wv, *ks)


def flash_kernel(at_ref, ka_ref, kb_ref, va_ref, vb_ref, *refs, heads, n_lo, n_hi, shifts):
    qs, out_ref = refs[:n_lo // 2], refs[n_lo // 2]
    q_scr, o_scr, lse_scr, bias = refs[n_lo // 2 + 1:]
    h = pl.program_id(0)
    hi, lo = at_ref[0], at_ref[1]
    block = qs[0].shape[1]
    tile = 2 * block
    n_y = n_lo // 2
    scale = (NOPE + ROPE) ** (-0.5)

    def place(i, m):
        row = lax.rem(lo // 2 - (0, 1, n_y - 1, 2)[i] + n_y, n_y)
        side = lax.rem(lo, 2)
        return row * 2 + (1 - side if m else side)

    @pl.when(h == 0)
    def _():
        lse_scr[...] = jnp.zeros_like(lse_scr)
        zero = jnp.zeros((block, 128 - NOPE - ROPE), BF16)
        gap = iota((block, block), 0) - iota((block, block), 1)
        for i in range(n_y):
            for m in range(2):
                rows = pl.ds(i * tile + m * block, block)
                for g in range(heads):
                    base = heads * NOPE + g * ROPE
                    plain = qs[i][m, :, g * NOPE:(g + 1) * NOPE]
                    turned = qs[i][m, :, base:base + ROPE]
                    q_scr[g, rows, :] = jnp.concatenate([plain, turned, zero], axis=1)
                first = hi * n_lo + place(i, m)
                for k, j in enumerate(shifts):
                    ahead = (lax.rem(hi - j + n_hi, n_hi) * n_lo + lo - first) * block
                    bias[rows, k * block:(k + 1) * block] = jnp.where(gap >= ahead, 0.0, -1e30)

    keys = jnp.concatenate([ka_ref[0], kb_ref[0]], axis=0)
    values = jnp.concatenate([va_ref[0], vb_ref[0]], axis=0)
    lane = iota((tile, 128), 1)
    for i in range(n_y):
        rows = pl.ds(i * tile, tile)
        s = dot_nt(q_scr[h, rows, :], keys) + bias[rows, :]
        top = jnp.max(s, axis=1, keepdims=True)
        p = jnp.exp2((s - top) * (scale * 1.4426950408889634)).astype(BF16)
        o = dot(p, values)
        total = o[:, VD:VD + 1]
        o_scr[h, rows, :] = (o * (1.0 / total)).astype(BF16)
        lse_scr[rows, :] = jnp.where(lane == h, top * scale + jnp.log(total), lse_scr[rows, :])

    @pl.when(h == heads - 1)
    def _():
        for i in range(n_y):
            for m in range(2):
                rows = pl.ds(i * tile + m * block, block)
                to = place(i, m)
                for g in range(heads):
                    out_ref[to, :, g * VD:(g + 1) * VD] = o_scr[g, rows, :VD]
                lse = lse_scr[rows, :]
                a = lse.astype(BF16).astype(F32)
                b = (lse - a).astype(BF16).astype(F32)
                c = lse - a - b
                packed = a + pltpu.roll(b, heads, axis=1) + pltpu.roll(c, 2 * heads, axis=1)
                out_ref[to, :, heads * VD:] = packed.astype(BF16)


def flash(at, qs, kx, vx, shifts):
    heads, keys, _ = kx[0].shape
    block = qs[0].shape[1]
    n_lo, n_hi = 2 * len(qs), len(shifts)
    rows = block * n_lo
    pair = pl.BlockSpec(qs[0].shape, lambda h, p: (0, 0, 0))
    shape = (n_lo, block, heads * VD + 128)
    return pl.pallas_call(
        functools.partial(flash_kernel, heads=heads, n_lo=n_lo, n_hi=n_hi, shifts=shifts),
        grid_spec=pltpu.PrefetchScalarGridSpec(
            num_scalar_prefetch=1,
            grid=(heads,),
            in_specs=[pl.BlockSpec((1, keys, 128), lambda h, p: (h, 0, 0))] * 4 + [pair] * len(qs),
            out_specs=pl.BlockSpec(shape, lambda h, p: (0, 0, 0)),
            scratch_shapes=[
                pltpu.VMEM((heads, rows, 128), BF16),
                pltpu.VMEM((heads, rows, 128), BF16),
                pltpu.VMEM((rows, 128), F32),
                pltpu.VMEM((rows, 2 * keys), F32),
            ],
        ),
        out_shape=jax.ShapeDtypeStruct(shape, BF16),
        name="flash",
        **params(8 * rows * keys * heads * 128, (rows * 2 + keys) * 640 * 2),
    )(at, *kx, *vx, *qs)


def merge_kernel(t_ref, parts_ref, wo_ref, *refs, heads):
    outs, scr = refs[:-1], refs[-1]
    n, rows = parts_ref.shape[:2]
    width = heads * VD
    lses = []
    for c in range(n):
        s = parts_ref[c, :, width:].astype(F32)
        lses.append(s + pltpu.roll(s, 128 - heads, axis=1) + pltpu.roll(s, 128 - 2 * heads, axis=1))
    top = functools.reduce(jnp.maximum, lses)
    factors = [jnp.exp(v - top) for v in lses]
    total = functools.reduce(jnp.add, factors)
    wide = jnp.where(iota((128, width), 1) // VD == iota((128, width), 0), 1.0, 0.0).astype(BF16)
    acc = jnp.zeros((rows, width), F32)
    for c in range(n):
        factor = factors[c] / total
        high = factor.astype(BF16)
        low = (factor - high.astype(F32)).astype(BF16)
        acc = acc + parts_ref[c, :, :width].astype(F32) * (dot(high, wide) + dot(low, wide))
    scr[...] = acc.astype(BF16)
    some = outs[0].shape[0]
    for j, out_ref in enumerate(outs):
        at = lax.rem(t_ref[2] + j, len(outs)) * some
        part = scr[pl.ds(pl.multiple_of(at, some), some), :]
        out_ref[...] = dot(part, wo_ref[...]).astype(BF16)


def merge(at, parts, wo, heads, n_tp):
    rows, width = parts.shape[1], wo.shape[1]
    vmem = pl.BlockSpec(memory_space=pltpu.VMEM)
    return pl.pallas_call(
        functools.partial(merge_kernel, heads=heads),
        in_specs=[pl.BlockSpec(memory_space=pltpu.SMEM)] + [vmem] * 2,
        out_specs=[vmem] * n_tp,
        out_shape=[jax.ShapeDtypeStruct((rows // n_tp, width), BF16)] * n_tp,
        scratch_shapes=[pltpu.VMEM((rows, heads * VD), BF16)],
        name="merge",
        **params(2 * rows * wo.shape[0] * width, wo.size * 2),
    )(at, parts, wo)


CHUNKS = 2


def round_tp(xs, n):
    up = [(i, (i + 1) % n) for i in range(n)]
    down = [(i, (i - 1) % n) for i in range(n)]
    sets = []
    for c, x in enumerate(xs):
        below = lax.ppermute(x, "tp", up)
        above = lax.ppermute(x, "tp", down)
        far = lax.ppermute(below, "tp", up) if c % 2 == 0 else lax.ppermute(above, "tp", down)
        sets.append((x, below, above, far))
    return sets


def swap_tp(xs, n):
    got = [xs[0]]
    for j in range(1, n):
        got.append(lax.ppermute(xs[j], "tp", [(i, (i + j) % n) for i in range(n)]))
    return got


def on_device(
    sizes,
    tokens_a,
    attn_gain,
    w_query,
    w_query_rot,
    w_latent,
    w_key_rot,
    latent_gain,
    w_key_up,
    w_value_up,
    w_output,
    tokens_b,
    ffn_gain,
    expert_ids,
    expert_weights,
    w_gate,
    w_up,
    w_down,
):
    n_hi, n_lo, n_tp = sizes
    n_ep = n_hi * n_lo
    hi, lo, tp = lax.axis_index("hi"), lax.axis_index("lo"), lax.axis_index("tp")
    at = jnp.stack([hi, lo, tp]).astype(jnp.int32)
    ep_axes = ("hi", "lo")

    rows_b, width = tokens_b.shape
    capacity = 2 * rows_b * expert_ids.shape[1] // n_ep
    part = width // n_tp
    outgoing, tgt = dispatch(at, tokens_b, ffn_gain, expert_ids, n_ep, capacity, 1, n_tp)
    arrived = lax.all_to_all(outgoing.reshape(n_ep, capacity, part), ep_axes, 0, 0, tiled=True)
    arrived = arrived.reshape(-1, part)

    wd = columns_of(at, w_down[0], n_tp)
    wd = swap_tp(wd, n_tp)

    rows_a = tokens_a.shape[0]
    heads = w_query.shape[1] // NOPE
    pos = ((hi * n_lo + lo) * rows_a + jnp.arange(rows_a, dtype=jnp.int32)).astype(F32)
    lane = jnp.arange(heads * ROPE, dtype=jnp.int32)
    half = ROPE // 2
    inverse = ROPE_BASE ** (-((lane % half).astype(F32) * 2.0) / ROPE)
    angles = pos[:, None] * inverse[None, :]
    cos = jnp.cos(angles)
    sin = jnp.where(lane % ROPE < half, -1.0, 1.0)[None, :] * jnp.sin(angles)
    q, kv = project(
        tokens_a, attn_gain, w_query, w_query_rot, w_latent, w_key_rot, latent_gain, cos, sin
    )

    other = [(i, i ^ 1) for i in range(n_lo)]
    up = [(i, (i + 2) % n_lo) for i in range(n_lo)]
    down = [(i, (i - 2) % n_lo) for i in range(n_lo)]
    q_other = lax.ppermute(q, "lo", other)
    pair = jnp.stack([q, q_other])
    q_below = lax.ppermute(pair, "lo", up)
    q_above = lax.ppermute(pair, "lo", down)
    q_far = lax.ppermute(q_below, "lo", up)

    def shifted(x, by):
        return lax.ppermute(x, "hi", [(i, (i + by) % n_hi) for i in range(n_hi)])

    ks = {0: kv}
    moves = ((1, 0, 1), (7, 0, -1), (2, 1, 1), (6, 7, -1), (3, 2, 1), (5, 6, -1), (4, 6, -2))
    for to, source, by in moves:
        ks[to] = shifted(ks[source], by)

    size = arrived.shape[0] // CHUNKS
    pieces = [arrived[c * size:(c + 1) * size] for c in range(CHUNKS)]
    chunks = [xs[1:] for xs in round_tp(pieces, n_tp)]
    h0 = hidden_of(at, n_tp, arrived, chunks, w_gate[0], w_up[0])
    t_up = [(i, (i + 1) % n_tp) for i in range(n_tp)]
    t_down = [(i, (i - 1) % n_tp) for i in range(n_tp)]
    hb = lax.ppermute(h0, "tp", t_up)
    ha = lax.ppermute(h0, "tp", t_down)
    fa = lax.ppermute(hb[:size], "tp", t_up)
    fb = lax.ppermute(ha[size:], "tp", t_down)
    done = down_of(h0, hb, ha, fa, fb, wd).reshape(n_ep, capacity, part)
    returned = lax.all_to_all(done, ep_axes, 0, 0, tiled=True).reshape(-1, part)
    high, low = shares_of(tgt.T, expert_weights, n_ep * capacity)
    mixed_b = combine(returned, high, low)

    near, rest = (0, 1, 7, 2), (6, 3, 5, 4)
    ka, va = expand([ks[j] for j in near], w_key_up, w_value_up)
    kb, vb = expand([ks[j] for j in rest], w_key_up, w_value_up)
    outs = flash(at, [pair, q_below, q_above, q_far], (ka, kb), (va, vb), near + rest)
    parts = lax.all_to_all(outs, "lo", 0, 0, tiled=True)
    partial = merge(at, parts, w_output, heads, n_tp)
    shared = swap_tp(partial, n_tp)
    mixed_a = functools.reduce(jnp.add, [v.astype(F32) for v in shared]).astype(BF16)
    return mixed_a, mixed_b


def solution(mesh):
    n_ep, n_tp = mesh.shape["ep"], mesh.shape["tp"]
    n_lo = 8
    n_hi = n_ep // n_lo
    grid = Mesh(mesh.devices.reshape(n_hi, n_lo, n_tp), ("hi", "lo", "tp"))
    ep = ("hi", "lo")
    placed = (
        P(ep, None),
        P(),
        P(None, "tp"),
        P(None, "tp"),
        P(),
        P(),
        P(),
        P(None, "tp"),
        P(None, "tp"),
        P("tp", None),
        P(ep, None),
        P(),
        P(ep, None),
        P(ep, None),
        P(ep, None, "tp"),
        P(ep, None, "tp"),
        P(ep, "tp", None),
    )

    def body(*args):
        return on_device((n_hi, n_lo, n_tp), *args)

    return jax.shard_map(
        body,
        mesh=grid,
        in_specs=placed,
        out_specs=(P(("hi", "lo", "tp"), None), P(ep, "tp")),
        check_vma=False,
    )
```
